32 devices in a mesh: ep: 8 (over z, x), tp: 4 (over y, core).
Axes of the slice: x: 2, y: 2, z: 4, core: 2. Of those that a mesh axis runs over, the one named last changes fastest.
Arguments:
- tokens: bfloat16 [2048, 2048], P('ep', 'tp'), may hold values from -6 to 6
- row_ids: int32 [2048, 16], P('ep'), may hold values from 0 to 32767, as said below
- row_gates: float32 [2048, 16], P('ep'), may hold values from 0.02 to 0.5
- key_table: bfloat16 [32768, 2048], P('ep', 'tp'), may hold values from -0.125 to 0.125
- value_table: bfloat16 [32768, 2048], P('ep', 'tp'), may hold values from -14 to 14
- norm_gain: float32 [2048], P('tp'), may hold values from 0.1 to 1.9
Outputs:
- output: bfloat16 [2048, 2048], P('ep', 'tp')
The draws below stay inside these ranges and needn't reach their ends.
Inputs may be any that keep to these rules, and one draw needn't show every extreme that they name: `row_ids`: table row r belongs to index r // 4096 of ep. The 256 tokens of one index of ep choose at most 1536 rows belonging to any one index, exactly 1536 from some index, and at least one from every index.
All inputs are finite; a program needn't handle non-finite values.
Results may differ from the reference program's by a relative error of at most 0.0065.
Values may be sent and summed in bfloat16 or wider, within the bound.
A program may use at most 64 MiB of HBM per device.

```python
import math
import jax
import jax.numpy as jnp
from jax import lax

D = 2048
PICKS = 16
EXP_DEV = 4096
TOK_DEV = 256
EXPERTS = 32768
TOKENS = 2048
CAP = 1536


def draw_row_ids(key, part):
    devices = TOKENS // TOK_DEV
    per_device = TOK_DEV * PICKS
    key_hot, key_order, key_local = jax.random.split(key, 3)
    hottest = jax.random.randint(key_hot, (devices, 1), 0, devices)
    slot = jnp.arange(per_device, dtype=jnp.int32)[None, :]
    spread = (slot - CAP) % (devices - 1)
    others = spread + (spread >= hottest).astype(jnp.int32)
    owner = jnp.where(slot < CAP, hottest, others)
    local = jax.random.randint(key_local, (devices, per_device), 0, EXP_DEV)
    order = jax.vmap(lambda k: jax.random.permutation(k, per_device))(jax.random.split(key_order, devices))
    chosen = jnp.take_along_axis(owner * EXP_DEV + local, order.astype(jnp.int32), axis=1)
    return chosen.reshape(TOKENS, PICKS).astype(jnp.int32)


def draw_value_table(key, part):
    key_base, key_rough = jax.random.split(key)
    column = jnp.arange(D, dtype=jnp.float32) / D
    rough = jax.random.uniform(key_rough, (D,), jnp.float32, 0.5, 1.5)
    base = jnp.clip(jax.random.normal(key_base, (EXPERTS, D), jnp.float32), -4.5, 4.5)
    rising = jnp.exp(math.log(4.0) * column)
    return (base * rising * rough * PICKS ** (-0.5)).astype(jnp.bfloat16)


def levels(stream_key, shape, pieces, least, high):
    level = 1.0
    for axis_at, blocks in pieces:
        steps = jax.random.uniform(jax.random.fold_in(jax.random.fold_in(stream_key, 6), axis_at), (blocks,), jnp.float32, least / len(pieces), high / len(pieces))
        level = level * jnp.repeat(jnp.exp(steps), shape[axis_at] // blocks).reshape((-1,) + (1,) * (len(shape) - 1 - axis_at))
    return level


def noise(key, dims, width, reach, pieces=(), held_as=jnp.bfloat16):
    array = width * jax.random.normal(key, dims, jnp.float32)
    if pieces:
        array = array * levels(key, dims, pieces, -0.22, 0.18)
    return jnp.clip(array, -reach, reach).astype(held_as)


def setup_inputs(seed: int = 0) -> dict:
    streams_of = jax.random.split(jax.random.key(seed), 7)
    return {
        "tokens": noise(streams_of[0], (TOKENS, D), 1.0, 6.0, ((0, 8), (1, 4))),
        "row_ids": draw_row_ids(jax.random.fold_in(streams_of[6], 71), 0),
        "row_gates": jnp.clip(jnp.exp(math.log(0.5) - 3.218876 * jax.random.uniform(streams_of[2], (TOKENS, PICKS), jnp.float32) ** levels(streams_of[2], (TOKENS, PICKS), ((0, 8),), -0.2, 0.2)), 0.02, 0.5),
        "key_table": noise(streams_of[3], (EXPERTS, D), D ** -0.5, 0.125, ((0, 8), (1, 4))),
        "value_table": draw_value_table(jax.random.fold_in(streams_of[6], 71), 0),
        "norm_gain": jnp.clip(1.0 + 0.18 * jax.random.normal(streams_of[5], (D,), jnp.float32), 0.1, 1.9),
    }


def reference(tokens, row_ids, row_gates, key_table, value_table, norm_gain):
    blocks = TOKENS // TOK_DEV

    def one_block(args):
        vectors, chosen, weights = args
        keys = key_table[chosen].astype(jnp.float32)
        score = jnp.einsum('td,tkd->tk', vectors.astype(jnp.float32), keys)
        hidden = jax.nn.gelu(score, approximate=False) * weights
        values = value_table[chosen].astype(jnp.float32)
        return jnp.einsum('tk,tkd->td', hidden, values)
    mixed = lax.map(one_block, (tokens.reshape(blocks, TOK_DEV, D), row_ids.reshape(blocks, TOK_DEV, PICKS), row_gates.reshape(blocks, TOK_DEV, PICKS)))
    mixed = mixed.reshape(TOKENS, D)
    strength = lax.optimization_barrier(jnp.mean(mixed * mixed, axis=-1, keepdims=True))
    return (mixed * lax.rsqrt(strength + 1e-06) * norm_gain).astype(jnp.bfloat16)
```

```python
import functools

import jax
import jax.numpy as jnp
from jax import lax
from jax.experimental import pallas as pl
from jax.experimental.pallas import tpu as pltpu
from jax.sharding import PartitionSpec as P

ROW = 256
LANES = 128
MESH = pl.DeviceIdType.MESH


def cycle_of(n):
    x = 1
    while 4 * x * x <= n:
        x *= 2
    z = n // x
    if x == 1 or z % 2:
        return list(range(n))
    out = []
    for row in range(z):
        cols = range(1, x) if row % 2 == 0 else range(x - 1, 0, -1)
        out += [row * x + col for col in cols]
    return out + [row * x for row in range(z - 1, -1, -1)]


def look(table, i):
    n = len(table)
    total = 0
    for k, v in enumerate(table):
        total = total + v * ((n * n - (i - k) * (i - k)) // (n * n))
    return total


def greet(n, tps, me, order):
    pos = look([order.index(i) for i in range(n)], me)
    right = look(order, lax.rem(pos + 1, n))
    left = look(order, lax.rem(pos + n - 1, n))
    mine = lax.axis_index("tp")
    barrier = pltpu.get_barrier_semaphore()
    for peer in (left, right):
        pl.semaphore_signal(barrier, inc=1, device_id=(peer, mine), device_id_type=MESH)
    for k in range(1, tps):
        pl.semaphore_signal(
            barrier, inc=1, device_id=(me, lax.rem(mine + k, tps)), device_id_type=MESH
        )
    pl.semaphore_wait(barrier, 2 + tps - 1)
    return pos, right, left, mine


def remote(src, dst, send, recv, device):
    return pltpu.make_async_remote_copy(
        src_ref=src, dst_ref=dst, send_sem=send, recv_sem=recv, device_id=device, device_id_type=MESH
    )


def score_kernel(n, tps, picks, order, chunks, *refs):
    x_ref, meta_ref, key_ref, hid_ref, meta_out, xall, s_ref, part, got_ref = refs[:9]
    xs, xr, ms, mr, ps, pr = refs[9:]
    block, width = x_ref.shape
    half = block // 2
    experts = key_ref.shape[0]
    rows = half // chunks
    me = lax.axis_index("ep")
    pos, right, left, mine = greet(n, tps, me, order)
    base = me * experts
    peers = (right, left)

    def x_copy(d, src_block, step, c, first):
        at = pl.ds(d * half + c * rows, rows)
        src = x_ref.at[at] if first else xall.at[src_block, at]
        return remote(
            src, xall.at[src_block, at], xs.at[d, step, c], xr.at[d, step, c], (peers[d], mine)
        )

    def m_copy(d, src_block, step, first):
        src = meta_ref.at[d] if first else meta_out.at[src_block, d]
        return remote(src, meta_out.at[src_block, d], ms.at[d, step], mr.at[d, step], (peers[d], mine))

    for d in (0, 1):
        m_copy(d, me, 0, True).start()
        for c in range(chunks):
            x_copy(d, me, 0, c, True).start()
    xall[me] = x_ref[...]
    meta_out[me] = meta_ref[...]

    per_half = LANES // picks
    sub = lax.broadcasted_iota(jnp.int32, (per_half, LANES), 0)
    lane = lax.broadcasted_iota(jnp.int32, (per_half, LANES), 1)
    own_lane = sub == lane // picks
    wide = min(512, experts)

    def step(s, carry):
        blocks = (look(order, lax.rem(pos + n - s, n)), look(order, lax.rem(pos + s, n)))

        @pl.when(s >= 1)
        def _():
            for d in (0, 1):
                m_copy(d, blocks[d], s - 1, False).wait_recv()

                @pl.when(s < n - 1)
                def _():
                    m_copy(d, blocks[d], s, False).start()

            for c in range(chunks):
                for d in (0, 1):
                    x_copy(d, blocks[d], s - 1, c, False).wait_recv()

                    @pl.when(s < n - 1)
                    def _():
                        x_copy(d, blocks[d], s, c, False).start()

        x = jnp.concatenate([xall[blocks[0], :half, :], xall[blocks[1], half:, :]], axis=0)
        for c in range(experts // wide):
            s_ref[:, c * wide : (c + 1) * wide] = lax.dot_general(
                x,
                key_ref[c * wide : (c + 1) * wide, :],
                (((1,), (1,)), ((), ())),
                preferred_element_type=jnp.float32,
            )
        for d in (0, 1):
            all_ids = meta_out[blocks[d], d, :8, :].astype(jnp.int32) - base
            for h2 in range(ROW // LANES):
                out = []
                for r in range(8):
                    ids = all_ids[r : r + 1, h2 * LANES : (h2 + 1) * LANES]
                    ids = jnp.broadcast_to(ids, (per_half, LANES))
                    owned = (ids >= 0) & (ids < experts)
                    hi = jnp.where(owned, ids >> 7, -1)
                    lo = jnp.where(owned, ids & (LANES - 1), 0)
                    row = d * half + r * (ROW // picks) + h2 * per_half
                    acc = jnp.zeros((per_half, LANES), jnp.float32)
                    for h in range(experts // LANES):
                        tile = s_ref[row : row + per_half, h * LANES : (h + 1) * LANES]
                        acc = jnp.where(hi == h, jnp.take_along_axis(tile, lo, axis=1), acc)
                    out.append(jnp.sum(jnp.where(own_lane, acc, 0.0), axis=0, keepdims=True))
                at = pl.multiple_of(blocks[d] * 16 + d * 8, 8)
                part[pl.ds(at, 8), h2 * LANES : (h2 + 1) * LANES] = jnp.concatenate(out, axis=0)
        return carry

    lax.fori_loop(0, n, step, 0)

    def p_copy(k):
        return remote(
            part, got_ref.at[k - 1], ps.at[k - 1], pr.at[k - 1], (me, lax.rem(mine + k, tps))
        )

    for k in range(1, tps):
        p_copy(k).start()

    def drain(s, carry):
        for d in (0, 1):
            m_copy(d, me, s, False).wait_send()
            for c in range(chunks):
                x_copy(d, me, s, c, False).wait_send()
        return carry

    lax.fori_loop(0, n - 1, drain, 0)
    for k in range(1, tps):
        p_copy(k).wait()
    total = part[...]
    for k in range(1, tps):
        total = total + got_ref[k - 1]
    hid_ref[...] = 0.5 * total * (1.0 + lax.erf(total * (0.5**0.5)))


def mix_kernel(n, tps, picks, order, *refs):
    h_ref, meta_ref, value_ref, gain_ref, out_ref, w_ref, sent, came, sq_ref, sq_got = refs[:10]
    ss, sr, qs, qr, out_total = refs[10:]
    experts, width = value_ref.shape
    block = out_ref.shape[0]
    half = block // 2
    me = lax.axis_index("ep")
    pos, right, left, mine = greet(n, tps, me, order)
    base = me * experts
    peers = (right, left)
    per = ROW // picks
    tall = experts // ROW * per
    lane_token = lax.broadcasted_iota(jnp.int32, (8, ROW), 1) // picks
    tall_iota = lax.broadcasted_iota(jnp.int32, (tall, ROW), 0)
    lo_iota = lax.broadcasted_iota(jnp.int32, (ROW, ROW), 0)

    def copy(d, s):
        return remote(sent.at[s, d], came.at[s, d], ss.at[d, s], sr.at[d, s], (peers[d], mine))

    def terms(s):
        blocks = (
            look(order, lax.rem(pos + 2 * n - 1 - s, n)),
            look(order, lax.rem(pos + 1 + s, n)),
        )
        for d in (0, 1):
            ids = meta_ref[blocks[d], d, :8, :].astype(jnp.int32) - base
            owned = (ids >= 0) & (ids < experts)
            codes = jnp.where(owned, (ids >> 8) * per + lane_token, -1)
            los = ids & (ROW - 1)
            at = pl.multiple_of(blocks[d] * 16 + d * 8, 8)
            hs = h_ref[pl.ds(at, 8), :] * meta_ref[blocks[d], d, 8:, :]
            for r in range(8):
                code, lo, h = codes[r : r + 1, :], los[r : r + 1, :], hs[r : r + 1, :]
                a = jnp.where(tall_iota == code, h, 0.0).astype(jnp.bfloat16)
                b = jnp.where(lo_iota == lo, 1.0, 0.0).astype(jnp.bfloat16)
                w = lax.dot_general(
                    a, b, (((1,), (1,)), ((), ())), preferred_element_type=jnp.float32
                ).astype(jnp.bfloat16)
                row = d * half + r * per
                for c in range(experts // ROW):
                    w_ref[row : row + per, c * ROW : (c + 1) * ROW] = w[c * per : (c + 1) * per, :]
        return jnp.dot(w_ref[...], value_ref[...], preferred_element_type=jnp.float32)

    def step(s, carry):
        out_total[...] = terms(s)
        for d in (0, 1):
            at = slice(d * half, (d + 1) * half)

            @pl.when(s >= 1)
            def _():
                copy(d, s - 1).wait_recv()
                out_total[at, :] = out_total[at, :] + came[s - 1, d].astype(jnp.float32)

            @pl.when(s < n - 1)
            def _():
                sent[s, d] = out_total[at, :].astype(jnp.bfloat16)
                copy(d, s).start()

        return carry

    lax.fori_loop(0, n, step, 0)
    mixed = out_total[...]
    ones = jnp.ones((8, width), jnp.float32)
    square = lax.dot_general(
        ones,
        mixed * mixed,
        (((1,), (1,)), ((), ())),
        precision=lax.Precision.HIGHEST,
        preferred_element_type=jnp.float32,
    )
    sq_ref[...] = square

    def q_copy(k):
        return remote(
            sq_ref, sq_got.at[k - 1], qs.at[k - 1], qr.at[k - 1], (me, lax.rem(mine + k, tps))
        )

    for k in range(1, tps):
        q_copy(k).start()

    def drain(s, carry):
        for d in (0, 1):
            copy(d, s).wait_send()
        return carry

    lax.fori_loop(0, n - 1, drain, 0)
    for k in range(1, tps):
        q_copy(k).wait()
    total = square
    for k in range(1, tps):
        total = total + sq_got[k - 1]
    scale = lax.rsqrt(total / (width * tps) + 1e-06)
    column = lax.dot_general(
        scale,
        jnp.full((8, LANES), 0.125, jnp.float32),
        (((0,), (0,)), ((), ())),
        precision=lax.Precision.HIGHEST,
        preferred_element_type=jnp.float32,
    )
    for c in range(width // LANES):
        at = slice(c * LANES, (c + 1) * LANES)
        out_ref[:, at] = (out_total[:, at] * column * gain_ref[:, at]).astype(jnp.bfloat16)


def body(tokens, row_ids, row_gates, key_table, value_table, norm_gain):
    block, width = tokens.shape
    picks = row_ids.shape[1]
    experts = key_table.shape[0]
    n, tps = lax.axis_size("ep"), lax.axis_size("tp")
    order = cycle_of(n)
    half = block // 2
    chunks = 2
    lines = half * picks // ROW
    meta = jnp.concatenate(
        [
            row_ids.astype(jnp.float32).reshape(2, lines, ROW),
            row_gates.reshape(2, lines, ROW),
        ],
        axis=1,
    )
    whole = pl.BlockSpec(memory_space=pltpu.VMEM)
    dma = pltpu.SemaphoreType.DMA
    hidden, metas = pl.pallas_call(
        functools.partial(score_kernel, n, tps, picks, order, chunks),
        out_shape=(
            jax.ShapeDtypeStruct((n * 2 * lines, ROW), jnp.float32),
            jax.ShapeDtypeStruct((n, 2, 2 * lines, ROW), jnp.float32),
        ),
        in_specs=[whole] * 3,
        out_specs=(whole, whole),
        scratch_shapes=[
            pltpu.VMEM((n, block, width), jnp.bfloat16),
            pltpu.VMEM((block, experts), jnp.float32),
            pltpu.VMEM((n * 2 * lines, ROW), jnp.float32),
            pltpu.VMEM((tps - 1, n * 2 * lines, ROW), jnp.float32),
            dma((2, n, chunks)),
            dma((2, n, chunks)),
            dma((2, n)),
            dma((2, n)),
            dma((tps - 1,)),
            dma((tps - 1,)),
        ],
        compiler_params=pltpu.CompilerParams(collective_id=0, has_side_effects=True),
    )(tokens, meta, key_table)
    return pl.pallas_call(
        functools.partial(mix_kernel, n, tps, picks, order),
        out_shape=jax.ShapeDtypeStruct((block, width), jnp.bfloat16),
        in_specs=[whole] * 4,
        out_specs=whole,
        scratch_shapes=[
            pltpu.VMEM((block, experts), jnp.bfloat16),
            pltpu.VMEM((n, 2, half, width), jnp.bfloat16),
            pltpu.VMEM((n, 2, half, width), jnp.bfloat16),
            pltpu.VMEM((8, block), jnp.float32),
            pltpu.VMEM((tps - 1, 8, block), jnp.float32),
            dma((2, n)),
            dma((2, n)),
            dma((tps - 1,)),
            dma((tps - 1,)),
            pltpu.VMEM((block, width), jnp.float32),
        ],
        compiler_params=pltpu.CompilerParams(collective_id=1, has_side_effects=True),
    )(hidden, metas, value_table, norm_gain.reshape(1, -1))


def solution(mesh):
    in_specs = (P("ep", "tp"), P("ep", None), P("ep", None), P("ep", "tp"), P("ep", "tp"), P("tp"))
    out_specs = P("ep", "tp")
    return jax.shard_map(body, mesh=mesh, in_specs=in_specs, out_specs=out_specs, check_vma=False)
```

```python
import functools

import jax
import jax.numpy as jnp
from jax import lax
from jax.experimental import pallas as pl
from jax.experimental.pallas import tpu as pltpu
from jax.sharding import PartitionSpec as P

ROW = 256
LANES = 128
MESH = pl.DeviceIdType.MESH


def cycle_of(n):
    x = 1
    while 4 * x * x <= n:
        x *= 2
    z = n // x
    if x == 1 or z % 2:
        return list(range(n))
    out = []
    for row in range(z):
        cols = range(1, x) if row % 2 == 0 else range(x - 1, 0, -1)
        out += [row * x + col for col in cols]
    return out + [row * x for row in range(z - 1, -1, -1)]


def look(table, i):
    n = len(table)
    total = 0
    for k, v in enumerate(table):
        total = total + v * ((n * n - (i - k) * (i - k)) // (n * n))
    return total


def greet(n, tps, me, order):
    pos = look([order.index(i) for i in range(n)], me)
    right = look(order, lax.rem(pos + 1, n))
    left = look(order, lax.rem(pos + n - 1, n))
    mine = lax.axis_index("tp")
    barrier = pltpu.get_barrier_semaphore()
    for peer in (left, right):
        pl.semaphore_signal(barrier, inc=1, device_id=(peer, mine), device_id_type=MESH)
    for k in range(1, tps):
        pl.semaphore_signal(
            barrier, inc=1, device_id=(me, lax.rem(mine + k, tps)), device_id_type=MESH
        )
    pl.semaphore_wait(barrier, 2 + tps - 1)
    return pos, right, left, mine


def remote(src, dst, send, recv, device):
    return pltpu.make_async_remote_copy(
        src_ref=src, dst_ref=dst, send_sem=send, recv_sem=recv, device_id=device, device_id_type=MESH
    )


def kernel(n, tps, picks, order, *refs):
    x_ref, meta_ref, key_hbm, value_hbm, gain_ref, out_ref = refs[:6]
    key_ref, value_ref, xall, metas, s_ref, part, got_ref, hid_ref, w_ref = refs[6:15]
    out_total, sent, came, sq_ref, sq_got = refs[15:20]
    xs, xr, ms, mr, ps, pr, ss, sr, qs, qr, kv = refs[20:]
    block, width = x_ref.shape
    half = block // 2
    experts = key_ref.shape[0]
    lines = meta_ref.shape[1] // 2
    rows = half // 2
    cuts = ss.shape[2]
    wide_out = width // cuts
    key_copy = pltpu.make_async_copy(key_hbm, key_ref, kv.at[0])
    value_copy = pltpu.make_async_copy(value_hbm, value_ref, kv.at[1])
    key_copy.start()
    me = lax.axis_index("ep")
    pos, right, left, mine = greet(n, tps, me, order)
    base = me * experts
    peers = (right, left)

    def x_copy(d, step, c, first=False):
        at = pl.ds(d * half + c * rows, rows)
        src = x_ref.at[at] if first else xall.at[step, at]
        return remote(
            src, xall.at[step + 1, at], xs.at[d, step, c], xr.at[d, step, c], (peers[d], mine)
        )

    def m_copy(d, step, first=False):
        src = meta_ref.at[d] if first else metas.at[step, d]
        return remote(src, metas.at[step + 1, d], ms.at[d, step], mr.at[d, step], (peers[d], mine))

    def p_copy(s, k):
        return remote(
            part.at[s],
            got_ref.at[s, k - 1],
            ps.at[s, k - 1],
            pr.at[s, k - 1],
            (me, lax.rem(mine + k, tps)),
        )

    for c in range(2):
        for d in (0, 1):
            x_copy(d, 0, c, True).start()
            if c == 0:
                m_copy(d, 0, True).start()
    xall[0] = x_ref[...]
    metas[0] = meta_ref[...]
    value_copy.start()
    key_copy.wait()

    per_half = LANES // picks
    sub = lax.broadcasted_iota(jnp.int32, (per_half, LANES), 0)
    lane = lax.broadcasted_iota(jnp.int32, (per_half, LANES), 1)
    own_lane = sub == lane // picks
    wide = min(512, experts)

    def pass_on(s, c):
        for d in (0, 1):
            x_copy(d, s - 1, c).wait_recv()

            @pl.when(s < n - 1)
            def _():
                x_copy(d, s, c).start()

            if c == 0:
                m_copy(d, s - 1).wait_recv()

                @pl.when(s < n - 1)
                def _():
                    m_copy(d, s).start()

    def choose(s):
        for d in (0, 1):
            all_ids = metas[s, d, :lines, :].astype(jnp.int32) - base
            for h2 in range(ROW // LANES):
                out = []
                for r in range(lines):
                    ids = all_ids[r : r + 1, h2 * LANES : (h2 + 1) * LANES]
                    ids = jnp.broadcast_to(ids, (per_half, LANES))
                    owned = (ids >= 0) & (ids < experts)
                    hi = jnp.where(owned, ids >> 7, -1)
                    lo = jnp.where(owned, ids & (LANES - 1), 0)
                    row = d * half + r * (ROW // picks) + h2 * per_half
                    acc = jnp.zeros((per_half, LANES), jnp.float32)
                    for h in range(experts // LANES):
                        tile = s_ref[row : row + per_half, h * LANES : (h + 1) * LANES]
                        acc = jnp.where(hi == h, jnp.take_along_axis(tile, lo, axis=1), acc)
                    out.append(jnp.sum(jnp.where(own_lane, acc, 0.0), axis=0, keepdims=True))
                part[s, d * lines : (d + 1) * lines, h2 * LANES : (h2 + 1) * LANES] = (
                    jnp.concatenate(out, axis=0)
                )
        for k in range(1, tps):
            p_copy(s, k).start()

    def score_step(s, carry):
        @pl.when((s >= 1) & (s < n))
        def _():
            pass_on(s, 0)

        @pl.when(s >= 1)
        def _():
            choose(s - 1)

        @pl.when((s >= 1) & (s < n))
        def _():
            pass_on(s, 1)

        @pl.when(s < n)
        def _():
            for c in range(experts // wide):
                s_ref[:, c * wide : (c + 1) * wide] = lax.dot_general(
                    xall[s],
                    key_ref[c * wide : (c + 1) * wide, :],
                    (((1,), (1,)), ((), ())),
                    preferred_element_type=jnp.float32,
                )

        return carry

    lax.fori_loop(0, n + 1, score_step, 0)
    value_copy.wait()

    per = ROW // picks
    tall = experts // ROW * per
    lane_token = lax.broadcasted_iota(jnp.int32, (lines, ROW), 1) // picks
    tall_iota = lax.broadcasted_iota(jnp.int32, (tall, ROW), 0)
    lo_iota = lax.broadcasted_iota(jnp.int32, (ROW, ROW), 0)

    def copy(d, s, c):
        return remote(
            sent.at[s, d, c], came.at[s, d, c], ss.at[d, s, c], sr.at[d, s, c], (peers[d], mine)
        )

    def mix_step(s, carry):
        slot = lax.rem(s + 1, n)
        total = part[slot]
        for k in range(1, tps):
            p_copy(slot, k).wait()
            total = total + got_ref[slot, k - 1]
        hid_ref[...] = 0.5 * total * (1.0 + lax.erf(total * (0.5**0.5)))
        for d in (0, 1):
            ids = metas[slot, d, :lines, :].astype(jnp.int32) - base
            owned = (ids >= 0) & (ids < experts)
            codes = jnp.where(owned, (ids >> 8) * per + lane_token, -1)
            los = ids & (ROW - 1)
            hs = hid_ref[d * lines : (d + 1) * lines, :] * metas[slot, d, lines:, :]
            for r in range(lines):
                code, lo, h = codes[r : r + 1, :], los[r : r + 1, :], hs[r : r + 1, :]
                a = jnp.where(tall_iota == code, h, 0.0).astype(jnp.bfloat16)
                b = jnp.where(lo_iota == lo, 1.0, 0.0).astype(jnp.bfloat16)
                w = lax.dot_general(
                    a, b, (((1,), (1,)), ((), ())), preferred_element_type=jnp.float32
                ).astype(jnp.bfloat16)
                row = d * half + r * per
                for c in range(experts // ROW):
                    w_ref[row : row + per, c * ROW : (c + 1) * ROW] = w[c * per : (c + 1) * per, :]
        for c in range(cuts):
            cols = slice(c * wide_out, (c + 1) * wide_out)
            out_total[:, cols] = jnp.dot(
                w_ref[...], value_ref[:, cols], preferred_element_type=jnp.float32
            )
            for d in (0, 1):
                at = slice(d * half, (d + 1) * half)

                @pl.when(s >= 1)
                def _():
                    copy(d, s - 1, c).wait_recv()
                    out_total[at, cols] = out_total[at, cols] + came[s - 1, d, c].astype(
                        jnp.float32
                    )

                @pl.when(s < n - 1)
                def _():
                    sent[s, d, c] = out_total[at, cols].astype(jnp.bfloat16)
                    copy(d, s, c).start()

        return carry

    lax.fori_loop(0, n, mix_step, 0)
    mixed = out_total[...]
    ones = jnp.ones((8, width), jnp.float32)
    square = lax.dot_general(
        ones,
        mixed * mixed,
        (((1,), (1,)), ((), ())),
        precision=lax.Precision.HIGHEST,
        preferred_element_type=jnp.float32,
    )
    sq_ref[...] = square

    def q_copy(k):
        return remote(
            sq_ref, sq_got.at[k - 1], qs.at[k - 1], qr.at[k - 1], (me, lax.rem(mine + k, tps))
        )

    for k in range(1, tps):
        q_copy(k).start()

    def drain(s, carry):
        for d in (0, 1):
            m_copy(d, s).wait_send()
            for c in range(2):
                x_copy(d, s, c).wait_send()
            for c in range(cuts):
                copy(d, s, c).wait_send()
        return carry

    lax.fori_loop(0, n - 1, drain, 0)
    for k in range(1, tps):
        q_copy(k).wait()
    total = square
    for k in range(1, tps):
        total = total + sq_got[k - 1]
    scale = lax.rsqrt(total / (width * tps) + 1e-06)
    column = lax.dot_general(
        scale,
        jnp.full((8, LANES), 0.125, jnp.float32),
        (((0,), (0,)), ((), ())),
        precision=lax.Precision.HIGHEST,
        preferred_element_type=jnp.float32,
    )
    for c in range(width // LANES):
        at = slice(c * LANES, (c + 1) * LANES)
        out_ref[:, at] = (out_total[:, at] * column * gain_ref[:, at]).astype(jnp.bfloat16)


def body(tokens, row_ids, row_gates, key_table, value_table, norm_gain):
    block, width = tokens.shape
    picks = row_ids.shape[1]
    experts = key_table.shape[0]
    n, tps = lax.axis_size("ep"), lax.axis_size("tp")
    half = block // 2
    lines = half * picks // ROW
    cuts = 2 if width % (2 * LANES) == 0 else 1
    meta = jnp.concatenate(
        [
            row_ids.astype(jnp.float32).reshape(2, lines, ROW),
            row_gates.reshape(2, lines, ROW),
        ],
        axis=1,
    )
    whole = pl.BlockSpec(memory_space=pltpu.VMEM)
    hbm = pl.BlockSpec(memory_space=pl.ANY)
    dma = pltpu.SemaphoreType.DMA
    bf16, f32 = jnp.bfloat16, jnp.float32
    return pl.pallas_call(
        functools.partial(kernel, n, tps, picks, cycle_of(n)),
        out_shape=jax.ShapeDtypeStruct((block, width), bf16),
        in_specs=[whole, whole, hbm, hbm, whole],
        out_specs=whole,
        scratch_shapes=[
            pltpu.VMEM((experts, width), bf16),
            pltpu.VMEM((experts, width), bf16),
            pltpu.VMEM((n, block, width), bf16),
            pltpu.VMEM((n, 2, 2 * lines, ROW), f32),
            pltpu.VMEM((block, experts), f32),
            pltpu.VMEM((n, 2 * lines, ROW), f32),
            pltpu.VMEM((n, tps - 1, 2 * lines, ROW), f32),
            pltpu.VMEM((2 * lines, ROW), f32),
            pltpu.VMEM((block, experts), bf16),
            pltpu.VMEM((block, width), f32),
            pltpu.VMEM((n - 1, 2, cuts, half, width // cuts), bf16),
            pltpu.VMEM((n - 1, 2, cuts, half, width // cuts), bf16),
            pltpu.VMEM((8, block), f32),
            pltpu.VMEM((tps - 1, 8, block), f32),
            dma((2, n - 1, 2)),
            dma((2, n - 1, 2)),
            dma((2, n - 1)),
            dma((2, n - 1)),
            dma((n, tps - 1)),
            dma((n, tps - 1)),
            dma((2, n - 1, cuts)),
            dma((2, n - 1, cuts)),
            dma((tps - 1,)),
            dma((tps - 1,)),
            dma((2,)),
        ],
        compiler_params=pltpu.CompilerParams(collective_id=0, has_side_effects=True),
    )(tokens, meta, key_table, value_table, norm_gain.reshape(1, -1))


def solution(mesh):
    in_specs = (P("ep", "tp"), P("ep", None), P("ep", None), P("ep", "tp"), P("ep", "tp"), P("tp"))
    out_specs = P("ep", "tp")
    return jax.shard_map(body, mesh=mesh, in_specs=in_specs, out_specs=out_specs, check_vma=False)
```
